32 devices in a mesh: ep: 4 (over y, x), tp: 8 (over z, core).
Axes of the slice: x: 2, y: 2, z: 4, core: 2. Of those that a mesh axis runs over, the one named last changes fastest.
Arguments:
- mix_in: bfloat16 [4096, 2048], P(('ep', 'tp')), may hold values from -6 to 6
- mix_gain: float32 [2048], replicated, may hold values from 0.1 to 1.9
- mix_w_in: bfloat16 [2048, 512], P('tp'), may hold values from -0.125 to 0.125
- pool_mat: bfloat16 [4, 128, 128], replicated, may hold values from -0.5 to 0.5
- pool_scale: float32 [512], replicated, may hold values from 0.1 to 1.9
- mix_w_out: bfloat16 [512, 2048], P(None, 'tp'), may hold values from -0.25 to 0.25
- moe_in: bfloat16 [4096, 2048], P(('ep', 'tp')), may hold values from -6 to 6
- moe_gain: float32 [2048], replicated, may hold values from 0.1 to 1.9
- routes: int32 [4096, 2], P('ep'), may hold values from 0 to 31, all different within a row; in each aligned block of 1024 rows (0 to 1023, 1024 to 2047, ...) at most 128 rows name the same one
- route_score: bfloat16 [4096, 2], P('ep'), may hold values from 0.099609375 to 1
- exp_gate: bfloat16 [32, 2048, 768], P(('ep', 'tp')), may hold values from -0.125 to 0.125
- exp_up: bfloat16 [32, 2048, 768], P(('ep', 'tp')), may hold values from -0.125 to 0.125
- exp_down: bfloat16 [32, 768, 2048], P(('ep', 'tp')), may hold values from -0.21875 to 0.21875
- shared_gate: bfloat16 [768, 2048], P('tp'), may hold values from -0.125 to 0.125
- shared_up: bfloat16 [768, 2048], P('tp'), may hold values from -0.125 to 0.125
- shared_down: bfloat16 [768, 2048], P('tp'), may hold values from -0.21875 to 0.21875
Outputs:
- mixed: bfloat16 [4096, 2048], P(('ep', 'tp'))
- moe_out: bfloat16 [4096, 2048], P(('ep', 'tp'))
The draws below stay inside these ranges and needn't reach their ends.
Inputs may be any that keep to these rules, and one draw needn't show every extreme that they name: `routes`: each row names 2 different experts. Within the rows of one index of ep (aligned blocks of 1024 rows) no expert is named more than 128 times, a bound that some expert reaches in some blocks.
All inputs are finite; a program needn't handle non-finite values.
Results may differ from the reference program's by a relative error of at most 0.012.
Values may be sent and summed in bfloat16 or wider, within the bound.
A program may use at most 128 MiB of HBM per device.

```python
import math
import jax
import jax.numpy as jnp
import numpy as np
from jax import lax

D = 2048
GROUP_CH = 128
POOL_GROUPS = 4
POOL = 512
FF = 768
FF_SH = 768
TOP_K = 2
SEQS_MIX = 1
TOK_MOE = 128
EXPERTS = 32
CAP = 128
TOKENS_MIX = 4096
LEN_MIX = 4096
TOKENS_MOE = 4096
N_EP = 4
N_TP = 8


def shard_levels(own_key, shape, shards, low, high):
    def one(axis_at, blocks):
        draws = jax.random.uniform(jax.random.fold_in(jax.random.fold_in(own_key, 6), axis_at), (blocks,), jnp.float32, low / len(shards), high / len(shards))
        return jnp.repeat(jnp.exp(draws), shape[axis_at] // blocks).reshape((-1,) + (1,) * (len(shape) - axis_at - 1))

    level = one(*shards[0])
    for cut in shards[1:]:
        level = level * one(*cut)
    return level


def deal_out(key, own, number, rows, number_of, top, reach, lean):
    sequence = jax.random.permutation(key, number_of)
    crowded, common = portions_of(number_of, rows * top, reach, lean, True), portions_of(number_of, rows * top, reach, lean, False)
    places = jnp.arange(number_of)

    def named(sizes, turn):
        used = int((sizes > 0).sum())
        fixed = max(1, used // 4)
        shifted = fixed + (places - fixed + turn * (used - fixed)) % max(1, number_of - fixed)
        return jnp.zeros((number_of,), jnp.int32).at[sequence[jnp.where(places < fixed, places, shifted)]].set(jnp.asarray(sizes, jnp.int32))

    sizes = jnp.where(number % 4 == 0, named(crowded, number // 4), named(common, number - number // 4 - 1))
    mixed = jax.random.permutation(jax.random.fold_in(own, 3), number_of)
    donor, taker = mixed[0:number_of // 2 * 2:2], mixed[1:number_of // 2 * 2:2]
    margin = jnp.minimum(sizes[donor] - 1, reach - sizes[taker]) // 2
    margin = jnp.where((donor == sequence[0]) | (taker == sequence[0]) | (sizes[taker] == 0), 0, jnp.maximum(margin, 0))
    shifted = jax.random.randint(jax.random.fold_in(own, 4), (number_of // 2,), 0, 1 << 20) % (margin + 1)
    sizes = sizes.at[donor].add(-shifted).at[taker].add(shifted)
    labels = jnp.searchsorted(jnp.cumsum(sizes), jnp.arange(rows * top), side="right").astype(jnp.int32)
    grid = labels.reshape(top, rows).T
    grid = grid[jax.random.permutation(jax.random.fold_in(own, 1), rows)]
    turn = jax.random.randint(jax.random.fold_in(own, 2), (rows, 1), 0, top)
    return jnp.take_along_axis(grid, (jnp.arange(top)[None, :] + turn) % top, axis=1)


def portions_of(amount, total, most, slope, full):
    weights = [(1 << 20) // math.isqrt(rank ** slope) + 1 for rank in range(1, amount + 1)]
    largest = most if full else min(most, max(-(-total // amount), total * weights[0] // sum(weights)))
    least = 1 if total - largest >= amount - 1 else 0
    given, surplus = [largest] + [least] * (amount - 1), total - largest - least * (amount - 1)
    while surplus > 0:
        candidates = [i for i in range(1, amount) if given[i] < largest] or [i for i in range(1, amount) if given[i] < most]
        mass, budget = sum([weights[i] for i in candidates]), surplus
        for i in candidates:
            addition = min(most - given[i], max(1, budget * weights[i] // mass), surplus)
            given[i] = given[i] + addition
            surplus = surplus - addition
    return np.array(given)


def normal_values(rng, shape, spread, most, split=(), kind=jnp.bfloat16):
    array = spread * jax.random.normal(rng, shape, jnp.float32)
    if split:
        array = array * shard_levels(rng, shape, split, -0.22, 0.18)
    return jnp.clip(array, -most, most).astype(kind)


def setup_inputs(seed: int = 0) -> dict:
    arg_keys = jax.random.split(jax.random.key(seed), 17)
    mix_in = normal_values(arg_keys[0], (TOKENS_MIX, D), 1.0, 6.0, ((0, 32),))
    mix_gain = jnp.clip(1.0 + 0.18 * jax.random.normal(arg_keys[1], (D,), jnp.float32), 0.1, 1.9)
    mix_w_in = normal_values(arg_keys[2], (D, POOL), D ** -0.5, 0.125, ((0, 8),))
    pool_mat = normal_values(arg_keys[3], (POOL_GROUPS, GROUP_CH, GROUP_CH), GROUP_CH ** -0.5, 0.5)
    pool_scale = jnp.clip(1.0 + 0.18 * jax.random.normal(arg_keys[4], (POOL,), jnp.float32), 0.1, 1.9)
    mix_w_out = normal_values(arg_keys[5], (POOL, D), POOL ** -0.5, 0.25, ((1, 8),))
    moe_in = normal_values(arg_keys[6], (TOKENS_MOE, D), 1.0, 6.0, ((0, 32),))
    moe_gain = jnp.clip(1.0 + 0.18 * jax.random.normal(arg_keys[7], (D,), jnp.float32), 0.1, 1.9)
    routes_keys = jax.random.split(jax.random.fold_in(arg_keys[8], 1), TOKENS_MOE // (TOK_MOE * N_TP))
    routes_turns = jax.random.permutation(jax.random.fold_in(arg_keys[8], 3), TOKENS_MOE // (TOK_MOE * N_TP))
    routes = jax.vmap(lambda own, number: deal_out(jax.random.fold_in(arg_keys[8], 2), own, number, TOK_MOE * N_TP, EXPERTS, TOP_K, CAP, 2))(routes_keys, routes_turns).reshape((TOKENS_MOE, TOP_K))
    route_score = jnp.clip(jnp.exp(math.log(1.0) - 2.306499 * jax.random.uniform(arg_keys[9], (TOKENS_MOE, TOP_K), jnp.float32) ** shard_levels(arg_keys[9], (TOKENS_MOE, TOP_K), ((0, 4),), -0.2, 0.2)), 0.099609375, 1.0).astype(jnp.bfloat16)
    exp_gate = normal_values(arg_keys[10], (EXPERTS, D, FF), D ** -0.5, 0.125, ((0, 32),))
    exp_up = normal_values(arg_keys[11], (EXPERTS, D, FF), D ** -0.5, 0.125, ((0, 32),))
    exp_down = normal_values(arg_keys[12], (EXPERTS, FF, D), FF ** -0.5, 0.21875, ((0, 32),))
    shared_gate = normal_values(arg_keys[13], (FF_SH, D), D ** -0.5, 0.125, ((0, 8),))
    shared_up = normal_values(arg_keys[14], (FF_SH, D), D ** -0.5, 0.125, ((0, 8),))
    shared_down = normal_values(arg_keys[15], (FF_SH, D), FF_SH ** -0.5, 0.21875, ((0, 8),))
    return dict(mix_in=mix_in, mix_gain=mix_gain, mix_w_in=mix_w_in, pool_mat=pool_mat, pool_scale=pool_scale, mix_w_out=mix_w_out, moe_in=moe_in, moe_gain=moe_gain, routes=routes, route_score=route_score, exp_gate=exp_gate, exp_up=exp_up, exp_down=exp_down, shared_gate=shared_gate, shared_up=shared_up, shared_down=shared_down)


NORM_EPS = 1e-06
ROUTED_SCALE = 2.5

def rms_rows(values, gain):
    floats = values.astype(jnp.float32)
    scaled = floats * lax.rsqrt(lax.optimization_barrier(jnp.mean(floats * floats, axis=-1, keepdims=True)) + NORM_EPS)
    return (scaled * gain.astype(jnp.float32)).astype(jnp.bfloat16)

def expert_ffn(rows_in, w_gate, w_up, w_down):
    gate_act = jnp.dot(rows_in, w_gate, preferred_element_type=jnp.float32)
    up_act = jnp.dot(rows_in, w_up, preferred_element_type=jnp.float32)
    hidden = (jax.nn.silu(gate_act) * up_act).astype(jnp.bfloat16)
    return jnp.dot(hidden, w_down, preferred_element_type=jnp.float32).astype(jnp.bfloat16)

def mixer_ref(mix_in, mix_gain, mix_w_in, pool_mat, pool_scale, mix_w_out):
    normed = rms_rows(mix_in, mix_gain)
    projected = jnp.dot(normed, mix_w_in, preferred_element_type=jnp.float32).astype(jnp.bfloat16)
    channels = projected.shape[1]
    reach_rows = 2 ** POOL_GROUPS - 1
    floats = projected.astype(jnp.float32).reshape(SEQS_MIX, LEN_MIX, channels)
    padded = jnp.pad(floats, ((0, 0), (reach_rows, 0), (0, 0)))
    position = jnp.arange(LEN_MIX, dtype=jnp.int32)
    pieces = []
    for group in range(POOL_GROUPS):
        window_len = 2 ** (group + 1)
        lower = group * GROUP_CH
        upper = lower + GROUP_CH
        running = jnp.zeros((SEQS_MIX, LEN_MIX, GROUP_CH), jnp.float32)
        for offset in range(window_len):
            running = running + padded[:, reach_rows - offset:reach_rows - offset + LEN_MIX, lower:upper]
        counts = jnp.minimum(position + 1, window_len).astype(jnp.float32)
        pieces.append(running / counts[None, :, None] - floats[:, :, lower:upper])
    pooled = jnp.concatenate(pieces, axis=2).astype(jnp.bfloat16).reshape(-1, POOL_GROUPS, GROUP_CH)
    grouped = jnp.einsum('tgc,gcd->tgd', pooled.astype(jnp.float32), pool_mat.astype(jnp.float32))
    pool_out = (grouped.reshape(-1, channels) * pool_scale).astype(jnp.bfloat16)
    return jnp.dot(pool_out, mix_w_out, preferred_element_type=jnp.float32).astype(jnp.bfloat16)

def experts_ref(moe_in, moe_gain, routes, route_score, exp_gate, exp_up, exp_down, shared_gate, shared_up, shared_down):
    normed = rms_rows(moe_in, moe_gain)
    total_rows, model_width = normed.shape
    block_rows = TOK_MOE * N_TP
    per_block = block_rows * TOP_K
    scores = route_score.astype(jnp.float32)
    weights = scores / lax.optimization_barrier(jnp.sum(scores, axis=1, keepdims=True)) * ROUTED_SCALE
    flat_expert = routes.reshape(N_EP, per_block)
    onehot = (flat_expert[:, :, None] == jnp.arange(EXPERTS, dtype=jnp.int32)[None, None, :]).astype(jnp.int32)
    before = lax.optimization_barrier(jnp.sum((jnp.cumsum(onehot, axis=1) - onehot) * onehot, axis=2))
    block_id = jnp.arange(N_EP, dtype=jnp.int32)[:, None]
    slot_span = N_EP * CAP
    flat_slot = (flat_expert * slot_span + block_id * CAP + before).reshape(-1).astype(jnp.int32)
    token_id = (block_id * block_rows + jnp.arange(per_block, dtype=jnp.int32)[None, :] // TOP_K).reshape(-1)
    table = jnp.full((EXPERTS * slot_span,), total_rows, jnp.int32).at[flat_slot].set(token_id)
    table = table.reshape(EXPERTS, slot_span)
    table_weight = jnp.zeros((EXPERTS * slot_span,), jnp.float32).at[flat_slot].set(weights.reshape(-1))
    table_weight = table_weight.reshape(EXPERTS, slot_span)
    padded_rows = jnp.concatenate([normed, jnp.zeros((1, model_width), jnp.bfloat16)], axis=0)
    gate_act = jnp.dot(normed, shared_gate.T, preferred_element_type=jnp.float32)
    up_act = jnp.dot(normed, shared_up.T, preferred_element_type=jnp.float32)
    shared_hidden = (jax.nn.silu(gate_act) * up_act).astype(jnp.bfloat16)
    shared_out = jnp.dot(shared_hidden, shared_down, preferred_element_type=jnp.float32)

    def column_sum(running, column):

        def one_expert(partial_value, ep_rank):
            expert = ep_rank * N_TP + column
            ids = table[expert]
            rows_in = jnp.take(padded_rows, ids, axis=0)
            outputs = expert_ffn(rows_in, exp_gate[expert], exp_up[expert], exp_down[expert])
            partial_value = partial_value.at[ids].add(outputs.astype(jnp.float32) * table_weight[expert][:, None], mode='drop')
            return (partial_value, None)
        partial_value = jnp.zeros((total_rows, model_width), jnp.float32)
        partial_value, _ = lax.scan(one_expert, partial_value, jnp.arange(N_EP, dtype=jnp.int32))
        return (running + partial_value.astype(jnp.bfloat16).astype(jnp.float32), None)
    running, _ = lax.scan(column_sum, jnp.zeros((total_rows, model_width), jnp.float32), jnp.arange(N_TP, dtype=jnp.int32))
    return (running + shared_out).astype(jnp.bfloat16)

def reference(mix_in, mix_gain, mix_w_in, pool_mat, pool_scale, mix_w_out, moe_in, moe_gain, routes, route_score, exp_gate, exp_up, exp_down, shared_gate, shared_up, shared_down):
    mixed = mixer_ref(mix_in, mix_gain, mix_w_in, pool_mat, pool_scale, mix_w_out)
    moe_out = experts_ref(moe_in, moe_gain, routes, route_score, exp_gate, exp_up, exp_down, shared_gate, shared_up, shared_down)
    return (mixed, moe_out)
```

```python
import functools

import jax
import jax.numpy as jnp
from jax import lax
from jax.experimental import pallas as pl
from jax.experimental.pallas import tpu as pltpu
from jax.sharding import PartitionSpec as P

SEQS_MIX = 1
CORES = 2

NORM_EPS = 1e-06
ROUTED_SCALE = 2.5
MESH = pl.DeviceIdType.MESH


def rms_rows(values, gain):
    floats = values.astype(jnp.float32)
    scaled = floats * lax.rsqrt(jnp.mean(floats * floats, axis=-1, keepdims=True) + NORM_EPS)
    return (scaled * gain).astype(jnp.bfloat16)


def remote(src, dst, send_sem, recv_sem, device):
    return pltpu.make_async_remote_copy(
        src_ref=src,
        dst_ref=dst,
        send_sem=send_sem,
        recv_sem=recv_sem,
        device_id=device,
        device_id_type=MESH,
    )


def greet(devices):
    barrier = pltpu.get_barrier_semaphore()
    for device in devices:
        pl.semaphore_signal(barrier, inc=1, device_id=device, device_id_type=MESH)
    pl.semaphore_wait(barrier, len(devices))


class Place:
    def __init__(self, ep_count, tp_count):
        self.ep_count, self.tp_count = ep_count, tp_count
        self.chips = tp_count // CORES
        self.far = self.chips // 2
        self.ep, self.tp = lax.axis_index("ep"), lax.axis_index("tp")
        self.chip, self.core = self.tp // CORES, self.tp % CORES

    def at(self, step):
        return (self.chip + step + self.chips) % self.chips

    def column(self, step, core):
        return self.at(step) * CORES + core

    def side(self, way):
        return (self.ep, self.column(1 if way == 0 else -1, self.core))

    def sibling(self):
        return (self.ep, self.column(0, 1 - self.core))

    def peers(self):
        return [((self.ep + i) % self.ep_count, self.tp) for i in range(1, self.ep_count)]


def ring_keys(chips):
    far = chips // 2
    return [
        (way, dist, half)
        for dist in range(1, far + 1)
        for turn in range(2)
        for way, half in ((0, turn), (1, 1 - turn))
        if dist < far or half == way
    ]


class RingGather:
    def __init__(self, place, buf, send, recv):
        self.place, self.buf, self.send, self.recv = place, buf, send, recv
        self.rows = buf.shape[1] // 2
        self.keys = ring_keys(place.chips)
        self.started = []

    def view(self, step, core, half):
        return self.buf.at[self.place.column(step, core), pl.ds(half * self.rows, self.rows)]

    def push(self, key):
        way, dist, half = key
        n = self.keys.index(key)
        block = self.view(-(dist - 1) if way == 0 else dist - 1, self.place.core, half)
        self._go(block, n, self.place.side(way))

    def _go(self, block, n, device):
        copy = remote(block, block, self.send.at[n], self.recv.at[n], device)
        copy.start()
        self.started.append(copy)

    def _arrived(self, block, n, device):
        remote(block, block, self.send.at[n], self.recv.at[n], device).wait_recv()

    def start(self):
        for key in self.keys:
            if key[1] == 1:
                self.push(key)
        block = self.buf.at[self.place.tp]
        self._go(block, 2 * len(self.keys), self.place.sibling())

    def step(self, dist):
        for n, key in enumerate(self.keys):
            if key[1] != dist:
                continue
            way, _, half = key
            block = self.view(-dist if way == 0 else dist, self.place.core, half)
            self._arrived(block, n, self.place.side(way))
            if (way, dist + 1, half) in self.keys:
                self.push((way, dist + 1, half))
            self._go(block, len(self.keys) + n, self.place.sibling())

    def arrive(self):
        for n, (way, dist, half) in enumerate(self.keys):
            block = self.view(-dist if way == 0 else dist, 1 - self.place.core, half)
            self._arrived(block, len(self.keys) + n, self.place.sibling())
        block = self.buf.at[self.place.column(0, 1 - self.place.core)]
        self._arrived(block, 2 * len(self.keys), self.place.sibling())

    def close(self):
        for copy in self.started:
            copy.wait_send()


def dispatch_kernel(
    ep_count, tp_count, moe_in, gain, table, gate_up, down, w_in, w_out,
    received, shared, w_in_all, w_out_all,
    rows_all, outgoing,
    xs, xr, ins, inr, outs, outr, as_, ar,
):
    place = Place(ep_count, tp_count)
    greet([place.side(0), place.side(1), place.sibling()] + place.peers())
    me = place.tp
    rows, width = moe_in.shape
    rows_all[pl.ds(me, 1)] = rms_rows(moe_in[...], gain[...])[None]
    tokens = RingGather(place, rows_all, xs, xr)
    tokens.start()
    w_in_all[pl.ds(me, 1)] = w_in[...][None]
    w_out_all[pl.ds(me, 1)] = w_out[...][None]
    for dist in range(1, place.far + 1):
        tokens.step(dist)
    first = RingGather(place, w_in_all, ins, inr)
    second = RingGather(place, w_out_all, outs, outr)
    tokens.arrive()
    first.start()
    second.start()

    cut = 512
    slots = table.shape[0]
    capacity = slots // ep_count

    def pick(i, carry):
        columns = pl.ds(pl.multiple_of(i * cut, cut), cut)
        block = rows_all[:, :, columns].reshape(tp_count * rows, cut)
        picked = jnp.dot(table[...], block, preferred_element_type=jnp.float32)
        outgoing[:, :, columns] = picked.astype(jnp.bfloat16).reshape(ep_count, capacity, cut)
        return carry

    lax.fori_loop(0, width // cut, pick, 0)
    copies = []
    for i, (peer, column) in enumerate(place.peers()):
        copy = remote(
            outgoing.at[peer], received.at[place.ep], as_.at[i], ar.at[i], (peer, column)
        )
        copy.start()
        copies.append(copy)
    received[pl.ds(place.ep, 1)] = outgoing[pl.ds(place.ep, 1)]
    for dist in range(1, place.far + 1):
        first.step(dist)

    units = down.shape[0]

    def ffn(i, carry):
        block = rows_all[pl.ds(i * CORES, CORES)].reshape(CORES * rows, width)
        both = lax.dot_general(
            block, gate_up[...], (((1,), (1,)), ((), ())), preferred_element_type=jnp.float32
        )
        spread = both.shape[1] // 2
        hidden = (jax.nn.silu(both[:, :spread]) * both[:, spread:]).astype(jnp.bfloat16)
        result = jnp.dot(hidden, down[...], preferred_element_type=jnp.float32)
        shared[pl.ds(i * CORES, CORES)] = result.astype(jnp.bfloat16).reshape(CORES, rows, width)
        return carry

    lax.fori_loop(0, tp_count // CORES, ffn, 0)
    for dist in range(1, place.far + 1):
        second.step(dist)
    first.arrive()
    second.arrive()
    for i in range(1, ep_count):
        source = (place.ep - i + ep_count) % ep_count
        remote(
            received.at[source], received.at[source], as_.at[i - 1], ar.at[i - 1],
            (source, place.tp),
        ).wait_recv()
    for copy in copies:
        copy.wait_send()
    for gather in (tokens, first, second):
        gather.close()


def combine_kernel(
    ep_count, tp_count, seq_len, results, table, shared, mix_in, mix_gain, w_in, pool_mat,
    pool_scale, w_out,
    mixed, moe_out,
    returned, own, for_sibling, from_sibling, sums, arrived, tail, prior,
    as_, ar, hs, hr, ss, sr, rs, rr,
):
    place = Place(ep_count, tp_count)
    devices = ep_count * tp_count
    flat = place.ep * tp_count + place.tp
    after, before = (flat + 1) % devices, (flat + devices - 1) % devices
    after = (after // tp_count, after % tp_count)
    before = (before // tp_count, before % tp_count)
    greet([place.side(0), place.side(1), place.sibling(), after, before] + place.peers())
    copies = []
    for i, (peer, column) in enumerate(place.peers()):
        copy = remote(
            results.at[peer], returned.at[place.ep], as_.at[i], ar.at[i], (peer, column)
        )
        copy.start()
        copies.append(copy)
    returned[pl.ds(place.ep, 1)] = results[pl.ds(place.ep, 1)]

    rows, width = mix_in.shape
    groups, group_ch = pool_mat.shape[0], pool_mat.shape[1]
    reach = 2**groups
    normed = rms_rows(mix_in[...], mix_gain[...])
    projected = jnp.dot(
        normed, w_in[...].reshape(width, groups * group_ch), preferred_element_type=jnp.float32
    ).astype(jnp.bfloat16)
    tail[...] = projected[rows - reach :]
    halo = remote(tail, prior, hs, hr, after)
    halo.start()
    halo.wait()
    first_row = flat * rows
    keep = jnp.where(first_row % seq_len == 0, 0.0, 1.0)
    extended = jnp.concatenate(
        [prior[...].astype(jnp.float32) * keep, projected.astype(jnp.float32)], axis=0
    )
    position = (first_row + lax.broadcasted_iota(jnp.int32, (rows, group_ch), 0)) % seq_len
    pieces = []
    for group in range(groups):
        channels = slice(group * group_ch, (group + 1) * group_ch)
        running = extended[:, channels]
        for level in range(group + 1):
            running = running + pltpu.roll(running, 2**level, 0)
        counts = jnp.minimum(position + 1, 2 ** (group + 1)).astype(jnp.float32)
        pooled = (running[reach:] / counts - extended[reach:, channels]).astype(jnp.bfloat16)
        grouped = jnp.dot(pooled, pool_mat[group], preferred_element_type=jnp.float32)
        pieces.append((grouped * pool_scale[:, channels]).astype(jnp.bfloat16))
    pool_out = jnp.concatenate(pieces, axis=1)
    span = w_out.shape[2]
    for column in range(tp_count):
        mixed[:, column * span : (column + 1) * span] = jnp.dot(
            pool_out, w_out[column], preferred_element_type=jnp.float32
        ).astype(jnp.bfloat16)

    for i in range(1, ep_count):
        source = (place.ep - i + ep_count) % ep_count
        remote(
            returned.at[source], returned.at[source], as_.at[i - 1], ar.at[i - 1],
            (source, place.tp),
        ).wait_recv()

    slots = table.shape[2]
    order = [place.far]
    for dist in range(place.far - 1, 0, -1):
        order += [dist, -dist]
    order += [0]
    cut = 512

    def total(step):
        chip = place.at(step)
        block = table[pl.ds(chip * CORES, CORES)].reshape(CORES * rows, slots)

        def part(i, carry):
            columns = pl.ds(pl.multiple_of(i * cut, cut), cut)
            values = jnp.dot(
                block,
                returned[:, :, columns].reshape(slots, cut),
                preferred_element_type=jnp.float32,
            ).reshape(CORES, rows, cut)
            values = values + shared[pl.ds(chip * CORES, CORES), :, columns].astype(jnp.float32)
            mine = jnp.where(place.core == 0, 1.0, 0.0)
            low, high = values[0], values[1]
            own[pl.ds(chip, 1), :, columns] = (low * mine + high * (1.0 - mine))[None]
            other = low * (1.0 - mine) + high * mine
            for_sibling[pl.ds(chip, 1), :, columns] = other.astype(jnp.bfloat16)[None]
            return carry

        lax.fori_loop(0, width // cut, part, 0)

    half_rows = rows // 2
    keys = ring_keys(place.chips)
    moves = []
    for n, step in enumerate(order):
        total(step)
        chip = place.at(step)
        copy = remote(
            for_sibling.at[chip], from_sibling.at[chip], ss.at[n], sr.at[n], place.sibling()
        )
        copy.start()
        moves.append(copy)

    def landed(key):
        way, dist, half = key
        n = keys.index(key)
        block = arrived.at[n]
        remote(block, block, rs.at[n], rr.at[n], place.side(way)).wait_recv()
        return arrived[n].astype(jnp.float32)

    for n, step in enumerate(order):
        chip = place.at(step)
        block = from_sibling.at[chip]
        remote(block, block, ss.at[n], sr.at[n], place.sibling()).wait_recv()
        dist = abs(step)
        if dist == 0:
            continue
        ways = (0, 1) if dist == place.far else ((0,) if step > 0 else (1,))
        for way, d, half in keys:
            if d != dist or way not in ways:
                continue
            span_rows = pl.ds(half * half_rows, half_rows)
            value = own[pl.ds(chip, 1), span_rows] + from_sibling[
                pl.ds(chip, 1), span_rows
            ].astype(jnp.float32)
            if (way, dist + 1, half) in keys:
                value = value + landed((way, dist + 1, half))[None]
            k = keys.index((way, dist, half))
            sums[pl.ds(k, 1)] = value.astype(jnp.bfloat16)
            copy = remote(sums.at[k], arrived.at[k], rs.at[k], rr.at[k], place.side(way))
            copy.start()
            moves.append(copy)
    for half in range(2):
        span_rows = pl.ds(half * half_rows, half_rows)
        value = own[pl.ds(place.chip, 1), span_rows] + from_sibling[
            pl.ds(place.chip, 1), span_rows
        ].astype(jnp.float32)
        value = value[0]
        for way in range(2):
            if (way, 1, half) in keys:
                value = value + landed((way, 1, half))
        moe_out[half * half_rows : (half + 1) * half_rows, :] = value.astype(jnp.bfloat16)
    for copy in copies + moves:
        copy.wait_send()


def vmem(count):
    return [pl.BlockSpec(memory_space=pltpu.VMEM)] * count


def shards(
    mix_in, mix_gain, mix_w_in, pool_mat, pool_scale, mix_w_out, moe_in, moe_gain, routes,
    route_score, exp_gate, exp_up, exp_down, shared_gate, shared_up, shared_down,
):
    ep_count, tp_count = lax.axis_size("ep"), lax.axis_size("tp")
    rows, width = moe_in.shape
    block_rows, top_count = routes.shape
    capacity = 2 * block_rows * top_count // (ep_count * tp_count)
    slots = ep_count * capacity
    dma = lambda n: pltpu.SemaphoreType.DMA((n,))
    bf16 = jnp.bfloat16
    messages = len(ring_keys(tp_count // CORES))

    column = lax.axis_index("tp")
    scores = route_score.astype(jnp.float32)
    weights = scores / jnp.sum(scores, axis=1, keepdims=True) * ROUTED_SCALE
    names = lax.iota(jnp.int32, ep_count) * tp_count + column
    hit = routes[:, :, None] == names[None, None, :]
    named = jnp.any(hit, axis=1)
    weight = jnp.sum(jnp.where(hit, weights[:, :, None], 0.0), axis=1)
    counted = named.astype(jnp.int32)
    spot = jnp.where(named, jnp.cumsum(counted, axis=0) - counted, -1)
    slot = lax.iota(jnp.int32, capacity)
    pick_table = (
        (spot.T[:, None, :] == slot[None, :, None]).astype(bf16).reshape(slots, block_rows)
    )
    sum_table = jnp.where(
        spot[:, :, None] == slot[None, None, :], weight[:, :, None], 0.0
    ).astype(bf16).reshape(tp_count, rows, slots)
    units = shared_gate.shape[0]
    spread = -(-units // 128) * 128
    pad = ((0, spread - units), (0, 0))
    gate_up = jnp.concatenate([jnp.pad(shared_gate, pad), jnp.pad(shared_up, pad)], axis=0)
    down = jnp.pad(shared_down, pad)

    received, shared, w_in_all, w_out_all = pl.pallas_call(
        functools.partial(dispatch_kernel, ep_count, tp_count),
        out_shape=[
            jax.ShapeDtypeStruct((ep_count, capacity, width), bf16),
            jax.ShapeDtypeStruct((tp_count, rows, width), bf16),
            jax.ShapeDtypeStruct((tp_count,) + mix_w_in.shape, bf16),
            jax.ShapeDtypeStruct((tp_count,) + mix_w_out.shape, bf16),
        ],
        in_specs=vmem(7),
        out_specs=vmem(4),
        scratch_shapes=[
            pltpu.VMEM((tp_count, rows, width), bf16),
            pltpu.VMEM((ep_count, capacity, width), bf16),
        ]
        + [dma(2 * messages + 1) for _ in range(6)]
        + [dma(ep_count - 1) for _ in range(2)],
        compiler_params=pltpu.CompilerParams(collective_id=0, has_side_effects=True),
    )(moe_in, moe_gain[None, :], pick_table, gate_up, down, mix_w_in, mix_w_out)

    flat_rows = received.reshape(slots, width)
    gate_act = jnp.dot(flat_rows, exp_gate[0], preferred_element_type=jnp.float32)
    up_act = jnp.dot(flat_rows, exp_up[0], preferred_element_type=jnp.float32)
    hidden = (jax.nn.silu(gate_act) * up_act).astype(bf16)
    results = jnp.dot(hidden, exp_down[0], preferred_element_type=jnp.float32).astype(bf16)

    chips = tp_count // CORES
    reach = 2 ** pool_mat.shape[0]
    channels = mix_w_in.shape[1]
    seq_len = mix_in.shape[0] * ep_count * tp_count // SEQS_MIX
    mixed, moe_out = pl.pallas_call(
        functools.partial(combine_kernel, ep_count, tp_count, seq_len),
        out_shape=[
            jax.ShapeDtypeStruct(mix_in.shape, bf16),
            jax.ShapeDtypeStruct(moe_in.shape, bf16),
        ],
        in_specs=vmem(9),
        out_specs=vmem(2),
        scratch_shapes=[
            pltpu.VMEM((ep_count, capacity, width), bf16),
            pltpu.VMEM((chips, rows, width), jnp.float32),
            pltpu.VMEM((chips, rows, width), bf16),
            pltpu.VMEM((chips, rows, width), bf16),
            pltpu.VMEM((messages, rows // 2, width), bf16),
            pltpu.VMEM((messages, rows // 2, width), bf16),
            pltpu.VMEM((reach, channels), bf16),
            pltpu.VMEM((reach, channels), bf16),
            dma(ep_count - 1),
            dma(ep_count - 1),
            pltpu.SemaphoreType.DMA,
            pltpu.SemaphoreType.DMA,
            dma(chips),
            dma(chips),
            dma(messages),
            dma(messages),
        ],
        compiler_params=pltpu.CompilerParams(collective_id=1, has_side_effects=True),
    )(
        results.reshape(ep_count, capacity, width), sum_table, shared, mix_in,
        mix_gain[None, :], w_in_all, pool_mat, pool_scale[None, :], w_out_all,
    )
    return (mixed, moe_out)


def solution(mesh):
    return jax.shard_map(
        shards,
        mesh=mesh,
        in_specs=(
            P(("ep", "tp"), None),
            P(),
            P("tp", None),
            P(),
            P(),
            P(None, "tp"),
            P(("ep", "tp"), None),
            P(),
            P("ep", None),
            P("ep", None),
            P(("ep", "tp"), None, None),
            P(("ep", "tp"), None, None),
            P(("ep", "tp"), None, None),
            P("tp", None),
            P("tp", None),
            P("tp", None),
        ),
        out_specs=(P(("ep", "tp"), None), P(("ep", "tp"), None)),
        check_vma=False,
    )
```

```python
import functools

import jax
import jax.numpy as jnp
from jax import lax
from jax.experimental import pallas as pl
from jax.experimental.pallas import tpu as pltpu
from jax.sharding import PartitionSpec as P

SEQS_MIX = 1
CORES = 2

NORM_EPS = 1e-06
ROUTED_SCALE = 2.5
MESH = pl.DeviceIdType.MESH


def rms_rows(values, gain):
    floats = values.astype(jnp.float32)
    scaled = floats * lax.rsqrt(jnp.mean(floats * floats, axis=-1, keepdims=True) + NORM_EPS)
    return (scaled * gain).astype(jnp.bfloat16)


def remote(src, dst, send_sem, recv_sem, device):
    return pltpu.make_async_remote_copy(
        src_ref=src,
        dst_ref=dst,
        send_sem=send_sem,
        recv_sem=recv_sem,
        device_id=device,
        device_id_type=MESH,
    )


def greet(devices):
    barrier = pltpu.get_barrier_semaphore()
    for device in devices:
        pl.semaphore_signal(barrier, inc=1, device_id=device, device_id_type=MESH)
    pl.semaphore_wait(barrier, len(devices))


class Place:
    def __init__(self, ep_count, tp_count):
        self.ep_count, self.tp_count = ep_count, tp_count
        self.chips = tp_count // CORES
        self.far = self.chips // 2
        self.ep, self.tp = lax.axis_index("ep"), lax.axis_index("tp")
        self.chip, self.core = self.tp // CORES, self.tp % CORES

    def at(self, step):
        return (self.chip + step + self.chips) % self.chips

    def column(self, step, core):
        return self.at(step) * CORES + core

    def side(self, way):
        return (self.ep, self.column(1 if way == 0 else -1, self.core))

    def sibling(self):
        return (self.ep, self.column(0, 1 - self.core))

    def peers(self):
        return [((self.ep + i) % self.ep_count, self.tp) for i in range(1, self.ep_count)]


def ring_keys(chips):
    far = chips // 2
    return [
        (way, dist, half)
        for dist in range(1, far + 1)
        for turn in range(2)
        for way, half in ((0, turn), (1, 1 - turn))
        if dist < far or half == way
    ]


class RingGather:
    def __init__(self, place, buf, send, recv):
        self.place, self.buf, self.send, self.recv = place, buf, send, recv
        self.rows = buf.shape[1] // 2
        self.keys = ring_keys(place.chips)
        self.started = []

    def view(self, step, core, half):
        return self.buf.at[self.place.column(step, core), pl.ds(half * self.rows, self.rows)]

    def push(self, key):
        way, dist, half = key
        n = self.keys.index(key)
        block = self.view(-(dist - 1) if way == 0 else dist - 1, self.place.core, half)
        self._go(block, n, self.place.side(way))

    def _go(self, block, n, device):
        copy = remote(block, block, self.send.at[n], self.recv.at[n], device)
        copy.start()
        self.started.append(copy)

    def _arrived(self, block, n, device):
        remote(block, block, self.send.at[n], self.recv.at[n], device).wait_recv()

    def start(self):
        for key in self.keys:
            if key[1] == 1:
                self.push(key)
        block = self.buf.at[self.place.tp]
        self._go(block, 2 * len(self.keys), self.place.sibling())

    def step(self, dist):
        for n, key in enumerate(self.keys):
            if key[1] != dist:
                continue
            way, _, half = key
            block = self.view(-dist if way == 0 else dist, self.place.core, half)
            self._arrived(block, n, self.place.side(way))
            if (way, dist + 1, half) in self.keys:
                self.push((way, dist + 1, half))
            self._go(block, len(self.keys) + n, self.place.sibling())

    def arrive(self):
        for n, (way, dist, half) in enumerate(self.keys):
            block = self.view(-dist if way == 0 else dist, 1 - self.place.core, half)
            self._arrived(block, len(self.keys) + n, self.place.sibling())
        block = self.buf.at[self.place.column(0, 1 - self.place.core)]
        self._arrived(block, 2 * len(self.keys), self.place.sibling())

    def close(self):
        for copy in self.started:
            copy.wait_send()


def layer_kernel(
    ep_count, tp_count, seq_len,
    moe_in, moe_gain, routes, scores, shared_gate, shared_up, shared_down, mix_w_in, mix_w_out,
    mix_in, mix_gain, pool_mat, pool_scale, exp_gate, exp_up, exp_down,
    mixed, moe_out,
    tokens, outgoing, received, results, returned, pick, share, total, w_in, w_out,
    gate_w, up_w, down_w, gate_sum, up_sum, from_sibling, sums, arrived, tail, prior,
    ws, xs, xr, ins, inr, outs, outr, as_, ar, bs, br, hs, hr, ss, sr, rs, rr,
):
    place = Place(ep_count, tp_count)
    devices = ep_count * tp_count
    flat = place.ep * tp_count + place.tp
    after, before = (flat + 1) % devices, (flat + devices - 1) % devices
    after = (after // tp_count, after % tp_count)
    before = (before // tp_count, before % tp_count)
    loads = [
        pltpu.make_async_copy(src.at[0], dst, ws.at[n])
        for n, (src, dst) in enumerate(((exp_gate, gate_w), (exp_up, up_w), (exp_down, down_w)))
    ]
    for load in loads:
        load.start()
    greet([place.side(0), place.side(1), place.sibling(), after, before] + place.peers())
    me = place.tp
    rows, width = moe_in.shape
    pieces, cut = tokens.shape[0], tokens.shape[3]
    capacity = outgoing.shape[2]
    slots = ep_count * capacity
    block_rows = tp_count * rows
    far = place.far
    sent = []

    normed = rms_rows(moe_in[...], moe_gain[...])
    for c in range(pieces):
        tokens[c, pl.ds(me, 1)] = normed[:, c * cut : (c + 1) * cut][None]
    gathers = [RingGather(place, tokens.at[c], xs.at[c], xr.at[c]) for c in range(pieces)]
    gathers[0].start()
    gathers[1].start()

    top_count = routes.shape[0]
    lines = max(8, ep_count)
    names = lax.broadcasted_iota(jnp.int32, (lines, block_rows), 0) * tp_count + me
    score_sum = jnp.sum(scores[...], axis=0, keepdims=True)
    named = jnp.zeros((lines, block_rows), jnp.float32)
    weight = jnp.zeros((lines, block_rows), jnp.float32)
    for k in range(top_count):
        hit = routes[k : k + 1, :] == names
        named = named + jnp.where(hit, 1.0, 0.0)
        weight = weight + jnp.where(hit, scores[k : k + 1, :] / score_sum * ROUTED_SCALE, 0.0)
    ones = named.astype(jnp.bfloat16)
    earlier = []
    for low in range(0, block_rows, 512):
        source = lax.broadcasted_iota(jnp.int32, (block_rows, 512), 0)
        target = lax.broadcasted_iota(jnp.int32, (block_rows, 512), 1) + low
        strict = jnp.where(source < target, 1.0, 0.0).astype(jnp.bfloat16)
        earlier.append(jnp.dot(ones, strict, preferred_element_type=jnp.float32))
    spot = jnp.where(named > 0.5, jnp.concatenate(earlier, axis=1), -1.0).astype(jnp.int32)
    slot = lax.broadcasted_iota(jnp.int32, (capacity, block_rows), 0)
    for j in range(ep_count):
        here = spot[j : j + 1, :] == slot
        span = slice(j * capacity, (j + 1) * capacity)
        pick[span, :] = jnp.where(here, 1.0, 0.0).astype(jnp.bfloat16)
        weighed = jnp.where(here, weight[j : j + 1, :], 0.0).T.astype(jnp.bfloat16)
        share[:, :, span] = weighed.reshape(tp_count, rows, capacity)

    def scatter(source, landing, c, send, recv):
        for i, (peer, column) in enumerate(place.peers()):
            copy = remote(
                source.at[c, peer], landing.at[c, place.ep], send.at[c, i], recv.at[c, i],
                (peer, column),
            )
            copy.start()
            sent.append(copy)
        landing[c, pl.ds(place.ep, 1)] = source[c, pl.ds(place.ep, 1)]

    def landing_wait(landing, c, send, recv):
        for i in range(1, ep_count):
            peer = (place.ep - i + ep_count) % ep_count
            block = landing.at[c, peer]
            remote(block, block, send.at[c, i - 1], recv.at[c, i - 1], (peer, me)).wait_recv()

    for c in range(pieces):
        for dist in range(1, far + 1):
            gathers[c].step(dist)
            if dist == 1 and c + 2 < pieces:
                gathers[c + 2].start()
        gathers[c].arrive()
        picked = jnp.dot(
            pick[...], tokens[c].reshape(block_rows, cut), preferred_element_type=jnp.float32
        )
        outgoing[c] = picked.astype(jnp.bfloat16).reshape(ep_count, capacity, cut)
        scatter(outgoing, received, c, as_, ar)

    w_in[pl.ds(me, 1)] = mix_w_in[...][None]
    w_out[pl.ds(me, 1)] = mix_w_out[...][None]
    first = RingGather(place, w_in, ins, inr)
    second = RingGather(place, w_out, outs, outr)
    first.start()
    second.start()

    def ffn(i, carry):
        across = (((1,), (1,)), ((), ()))
        pair = pl.ds(i * CORES, CORES)
        gate = jnp.zeros((CORES * rows, shared_gate.shape[0]), jnp.float32)
        up = gate
        for c in range(pieces):
            block = tokens[c, pair].reshape(CORES * rows, cut)
            span = slice(c * cut, (c + 1) * cut)
            gate = gate + lax.dot_general(
                block, shared_gate[:, span], across, preferred_element_type=jnp.float32
            )
            up = up + lax.dot_general(
                block, shared_up[:, span], across, preferred_element_type=jnp.float32
            )
        hidden = (jax.nn.silu(gate) * up).astype(jnp.bfloat16)
        for c in range(pieces):
            value = jnp.dot(
                hidden, shared_down[:, c * cut : (c + 1) * cut], preferred_element_type=jnp.float32
            )
            total[c, pair] = value.astype(jnp.bfloat16).reshape(CORES, rows, cut)
        return carry

    lax.fori_loop(0, tp_count // CORES, ffn, 0)

    for load in loads:
        load.wait()
    for c in range(pieces):
        landing_wait(received, c, as_, ar)
        block = received[c].reshape(slots, cut)
        for acc, weights in ((gate_sum, gate_w), (up_sum, up_w)):
            value = jnp.dot(
                block, weights[c * cut : (c + 1) * cut, :], preferred_element_type=jnp.float32
            )
            acc[...] = value if c == 0 else acc[...] + value
    hidden = (jax.nn.silu(gate_sum[...]) * up_sum[...]).astype(jnp.bfloat16)
    for c in range(pieces):
        value = jnp.dot(
            hidden, down_w[:, c * cut : (c + 1) * cut], preferred_element_type=jnp.float32
        )
        results[c] = value.astype(jnp.bfloat16).reshape(ep_count, capacity, cut)
        scatter(results, returned, c, bs, br)

    for dist in range(1, far + 1):
        first.step(dist)
        second.step(dist)

    order = [far]
    for dist in range(far - 1, 0, -1):
        order += [dist, -dist]
    order += [0]
    half_rows = rows // 2
    keys = ring_keys(place.chips)

    def halves(half):
        return pl.ds(half * half_rows, half_rows)

    def landed(c, key):
        n = keys.index(key)
        block = arrived.at[c, n]
        remote(block, block, rs.at[c, n], rr.at[c, n], place.side(key[0])).wait_recv()
        return arrived[c, n].astype(jnp.float32)

    def chip_sum(c, chip, half):
        mine = total[c, pl.ds(chip * CORES + place.core, 1), halves(half)]
        theirs = from_sibling[c, pl.ds(chip, 1), halves(half)]
        return (mine.astype(jnp.float32) + theirs.astype(jnp.float32))[0]

    def sibling_wait(c, n):
        block = from_sibling.at[c, place.at(order[n])]
        remote(block, block, ss.at[c, n], sr.at[c, n], place.sibling()).wait_recv()

    def pass_on(c, n):
        step = order[n]
        dist = abs(step)
        sibling_wait(c, n)
        ways = (0, 1) if dist == far else ((0,) if step > 0 else (1,))
        for k, (way, d, half) in enumerate(keys):
            if d != dist or way not in ways:
                continue
            value = chip_sum(c, place.at(step), half)
            if (way, dist + 1, half) in keys:
                value = value + landed(c, (way, dist + 1, half))
            sums[c, k] = value.astype(jnp.bfloat16)
            copy = remote(
                sums.at[c, k], arrived.at[c, k], rs.at[c, k], rr.at[c, k], place.side(way)
            )
            copy.start()
            sent.append(copy)

    for c in range(pieces):
        landing_wait(returned, c, bs, br)
        for n, step in enumerate(order):
            chip = place.at(step)
            pair = pl.ds(chip * CORES, CORES)
            value = jnp.dot(
                share[pair].reshape(CORES * rows, slots),
                returned[c].reshape(slots, cut),
                preferred_element_type=jnp.float32,
            ).reshape(CORES, rows, cut)
            total[c, pair] = (value + total[c, pair].astype(jnp.float32)).astype(jnp.bfloat16)
            copy = remote(
                total.at[c, chip * CORES + 1 - place.core], from_sibling.at[c, chip],
                ss.at[c, n], sr.at[c, n], place.sibling(),
            )
            copy.start()
            sent.append(copy)
        pass_on(c, 0)

    first.arrive()
    second.arrive()
    groups, group_ch = pool_mat.shape[0], pool_mat.shape[1]
    reach = 2**groups
    mix_normed = rms_rows(mix_in[...], mix_gain[...])
    projected = jnp.dot(
        mix_normed, w_in[...].reshape(width, groups * group_ch), preferred_element_type=jnp.float32
    ).astype(jnp.bfloat16)
    tail[...] = projected[rows - reach :]
    halo = remote(tail, prior, hs, hr, after)
    halo.start()
    for n in range(1, len(order) - 1):
        for c in range(pieces):
            pass_on(c, n)
    halo.wait()
    first_row = flat * rows
    keep = jnp.where(first_row % seq_len == 0, 0.0, 1.0)
    extended = jnp.concatenate(
        [prior[...].astype(jnp.float32) * keep, projected.astype(jnp.float32)], axis=0
    )
    position = (first_row + lax.broadcasted_iota(jnp.int32, (rows, group_ch), 0)) % seq_len
    pooled_parts = []
    for group in range(groups):
        channels = slice(group * group_ch, (group + 1) * group_ch)
        running = extended[:, channels]
        for level in range(group + 1):
            running = running + pltpu.roll(running, 2**level, 0)
        counts = jnp.minimum(position + 1, 2 ** (group + 1)).astype(jnp.float32)
        pooled = (running[reach:] / counts - extended[reach:, channels]).astype(jnp.bfloat16)
        grouped = jnp.dot(pooled, pool_mat[group], preferred_element_type=jnp.float32)
        pooled_parts.append((grouped * pool_scale[:, channels]).astype(jnp.bfloat16))
    pool_out = jnp.concatenate(pooled_parts, axis=1)
    span = w_out.shape[2]
    for column in range(tp_count):
        mixed[:, column * span : (column + 1) * span] = jnp.dot(
            pool_out, w_out[column], preferred_element_type=jnp.float32
        ).astype(jnp.bfloat16)

    for c in range(pieces):
        sibling_wait(c, len(order) - 1)
        for half in range(2):
            value = chip_sum(c, place.chip, half)
            for way in range(2):
                if (way, 1, half) in keys:
                    value = value + landed(c, (way, 1, half))
            moe_out[half * half_rows : (half + 1) * half_rows, c * cut : (c + 1) * cut] = (
                value.astype(jnp.bfloat16)
            )
    for copy in sent:
        copy.wait_send()
    for gather in gathers + [first, second]:
        gather.close()


def vmem(count):
    return [pl.BlockSpec(memory_space=pltpu.VMEM)] * count


def shards(
    mix_in, mix_gain, mix_w_in, pool_mat, pool_scale, mix_w_out, moe_in, moe_gain, routes,
    route_score, exp_gate, exp_up, exp_down, shared_gate, shared_up, shared_down,
):
    ep_count, tp_count = lax.axis_size("ep"), lax.axis_size("tp")
    rows, width = moe_in.shape
    block_rows, top_count = routes.shape
    capacity = 2 * block_rows * top_count // (ep_count * tp_count)
    slots = ep_count * capacity
    dma = lambda n: pltpu.SemaphoreType.DMA((n,))
    bf16 = jnp.bfloat16
    messages = len(ring_keys(tp_count // CORES))

    chips = tp_count // CORES
    pieces = 4
    cut = width // pieces
    hidden = exp_gate.shape[2]
    reach = 2 ** pool_mat.shape[0]
    seq_len = mix_in.shape[0] * ep_count * tp_count // SEQS_MIX
    grid = lambda n: pltpu.SemaphoreType.DMA((pieces, n))
    buffer = lambda *shape: pltpu.VMEM(shape, bf16)
    mixed, moe_out = pl.pallas_call(
        functools.partial(layer_kernel, ep_count, tp_count, seq_len),
        out_shape=[
            jax.ShapeDtypeStruct(mix_in.shape, bf16),
            jax.ShapeDtypeStruct(moe_in.shape, bf16),
        ],
        in_specs=vmem(13) + [pl.BlockSpec(memory_space=pl.ANY)] * 3,
        out_specs=vmem(2),
        scratch_shapes=[
            buffer(pieces, tp_count, rows, cut),
            buffer(pieces, ep_count, capacity, cut),
            buffer(pieces, ep_count, capacity, cut),
            buffer(pieces, ep_count, capacity, cut),
            buffer(pieces, ep_count, capacity, cut),
            buffer(slots, block_rows),
            buffer(tp_count, rows, slots),
            buffer(pieces, tp_count, rows, cut),
            buffer(tp_count, *mix_w_in.shape),
            buffer(tp_count, *mix_w_out.shape),
            buffer(width, hidden),
            buffer(width, hidden),
            buffer(hidden, width),
            pltpu.VMEM((slots, hidden), jnp.float32),
            pltpu.VMEM((slots, hidden), jnp.float32),
            buffer(pieces, chips, rows, cut),
            buffer(pieces, messages, rows // 2, cut),
            buffer(pieces, messages, rows // 2, cut),
            buffer(reach, mix_w_in.shape[1]),
            buffer(reach, mix_w_in.shape[1]),
            dma(3),
            grid(2 * messages + 1),
            grid(2 * messages + 1),
        ]
        + [dma(2 * messages + 1) for _ in range(4)]
        + [grid(ep_count - 1) for _ in range(4)]
        + [pltpu.SemaphoreType.DMA, pltpu.SemaphoreType.DMA]
        + [grid(chips), grid(chips), grid(messages), grid(messages)],
        compiler_params=pltpu.CompilerParams(
            collective_id=0, has_side_effects=True, vmem_limit_bytes=67043328
        ),
    )(
        moe_in, moe_gain[None, :], routes.T, route_score.T.astype(jnp.float32), shared_gate,
        shared_up, shared_down, mix_w_in, mix_w_out, mix_in, mix_gain[None, :], pool_mat,
        pool_scale[None, :], exp_gate, exp_up, exp_down,
    )
    return (mixed, moe_out)


def solution(mesh):
    return jax.shard_map(
        shards,
        mesh=mesh,
        in_specs=(
            P(("ep", "tp"), None),
            P(),
            P("tp", None),
            P(),
            P(),
            P(None, "tp"),
            P(("ep", "tp"), None),
            P(),
            P("ep", None),
            P("ep", None),
            P(("ep", "tp"), None, None),
            P(("ep", "tp"), None, None),
            P(("ep", "tp"), None, None),
            P("tp", None),
            P("tp", None),
            P("tp", None),
        ),
        out_specs=(P(("ep", "tp"), None), P(("ep", "tp"), None)),
        check_vma=False,
    )
```
